32 devices in a mesh: dp: 2 (over x), kv: 8 (over z, y), tp: 2 (over core).
Axes of the slice: x: 2, y: 2, z: 4, core: 2. Of those that a mesh axis runs over, the one named last changes fastest.
Arguments:
- tokens: bfloat16 [2, 1536, 2048], P('dp', 'kv'), may hold values from -60 to 60
- doc_lengths: int32 [2, 8], P('dp'), may hold values from 1 to 768, as said below
- picked: int32 [2, 48, 32], P('dp', 'kv'), may hold values from -1 to 47, as said below
- w_query: bfloat16 [2048, 1024], P(None, 'tp'), may hold values from -0.125 to 0.125
- w_key: bfloat16 [2048, 128], replicated, may hold values from -0.125 to 0.125
- w_value: bfloat16 [2048, 128], replicated, may hold values from -0.125 to 0.125
- w_out: bfloat16 [1024, 2048], replicated, may hold values from -0.1875 to 0.1875
Outputs:
- mixed: bfloat16 [2, 1536, 2048], P('dp', 'kv')
The draws below stay inside these ranges and needn't reach their ends.
Inputs may be any that keep to these rules, and one draw needn't show every extreme that they name: `doc_lengths`: each row sums to 1536; its largest document has exactly 768 positions. `picked`: slot 0 of query block b is b itself; the other slots hold distinct blocks before b, or -1 when fewer such blocks are named. Of the 6 blocks that one device of kv holds, at most 2 are named by query blocks held by other devices of kv, and in every row some device reaches 2.
All inputs are finite; a program needn't handle non-finite values.
Results may differ from the reference program's by a relative error of at most 0.011.
Values may be sent and summed in bfloat16 or wider, within the bound.
A program may use at most 64 MiB of HBM per device.

```python
import jax
import jax.numpy as jnp
from jax import lax

D = 2048
HEADS = 16
KV_HEADS = 2
HEAD_DIM = 64
BLOCK = 32
PICKS = 32
DOCS = 8
TOK_DEV = 192
GROUPS = 2
SEQ = 1536
NBLOCKS = 48


def pack_lengths(key):
    half = SEQ // 2

    def one_row(subkey):
        cuts = jnp.sort(jax.random.permutation(jax.random.fold_in(subkey, 1), half - 1)[:DOCS - 2].astype(jnp.int32) + 1)
        edges = jnp.concatenate([jnp.zeros((1,), jnp.int32), cuts, jnp.full((1,), half, jnp.int32)])
        small = edges[1:] - edges[:-1]
        place = jax.random.randint(jax.random.fold_in(subkey, 2), (), 0, DOCS)
        slot_ids = jnp.arange(DOCS, dtype=jnp.int32)
        before = jnp.concatenate([small, small[-1:]])
        after = jnp.concatenate([small[:1], small])
        return jnp.where(slot_ids < place, before, jnp.where(slot_ids == place, half, after)).astype(jnp.int32)
    subkeys = jax.random.split(jax.random.fold_in(key, 7), GROUPS)
    return jax.vmap(one_row)(subkeys)


def draw_doc_lengths(key, part):
    return pack_lengths(key)


def draw_picked(key, part):
    blocks_dev = TOK_DEV // BLOCK
    devices = NBLOCKS // blocks_dev
    midway = devices // 2

    def one_row(subkey):
        block_ids = jnp.arange(NBLOCKS, dtype=jnp.int32)
        owner = block_ids // blocks_dev
        within = block_ids % blocks_dev
        favored = jax.random.randint(jax.random.fold_in(subkey, 1), (devices,), 0, blocks_dev - 1).astype(jnp.int32)
        favored_block = favored[owner]
        hot_block = (within == blocks_dev - 1) | (within == favored_block)
        fame = jax.random.randint(jax.random.fold_in(subkey, 2), (devices,), 0, 4).astype(jnp.int32)[owner]
        base = jax.random.randint(jax.random.fold_in(subkey, 3), (NBLOCKS, NBLOCKS), 0, 1024).astype(jnp.int32)
        row_ids = block_ids[:, None]
        col_ids = block_ids[None, :]
        same_device = owner[:, None] == owner[None, :]
        allowed = (col_ids < row_ids) & (same_device | hot_block[None, :])
        previous = (col_ids == row_ids - 1).astype(jnp.int32) * 65536
        far_row = (owner[:, None] >= midway) & (within[:, None] == 0)
        far_col = (owner[None, :] == owner[:, None] - midway) & (within[None, :] == favored_block[None, :])
        far = (far_row & far_col).astype(jnp.int32) * 65536
        score = base + (fame * 1024)[None, :] + same_device.astype(jnp.int32) * 2048 + previous + far
        score = jnp.where(allowed, score * NBLOCKS + col_ids, -1)
        top_values, top_index = lax.top_k(score, PICKS - 1)
        others = jnp.where(top_values >= 0, top_index, -1)
        return jnp.concatenate([block_ids[:, None], others], axis=1).astype(jnp.int32)
    subkeys = jax.random.split(jax.random.fold_in(key, 11), GROUPS)
    return jax.vmap(one_row)(subkeys)


def draw_tokens(key, part):
    values = jax.random.normal(jax.random.fold_in(key, 3), (GROUPS, SEQ, D), jnp.float32)
    return jnp.clip(values, -60.0, 60.0).astype(jnp.bfloat16)


def block_scale(rng, extent, shards, smallest, high):
    level, own = 1.0, jax.random.fold_in(rng, 6)
    for position, parts in shards:
        draws = jnp.exp(jax.random.uniform(jax.random.fold_in(own, position), (parts,), jnp.float32, smallest / len(shards), high / len(shards)))
        level = level * jnp.repeat(draws, extent[position] // parts).reshape([-1 if axis == position else 1 for axis in range(len(extent))])
    return level


def bell_draw(rng, shape, scale, most, cuts=(), kind=jnp.bfloat16):
    values = jax.random.normal(rng, shape, jnp.float32) * scale
    if len(cuts) > 0:
        values = block_scale(rng, shape, cuts, -0.22, 0.18) * values
    return jnp.clip(values, min=-most, max=most).astype(kind)


def setup_inputs(seed: int = 0) -> dict:
    key_list = jax.random.split(jax.random.key(seed), 8)
    tokens = draw_tokens(jax.random.fold_in(key_list[7], 71), 0)
    doc_lengths = draw_doc_lengths(jax.random.fold_in(key_list[7], 71), 0)
    picked = draw_picked(jax.random.fold_in(key_list[7], 71), 0)
    w_query = bell_draw(key_list[3], (D, HEADS * HEAD_DIM), D ** -0.5, 0.125, ((1, 2),))
    w_key = bell_draw(key_list[4], (D, KV_HEADS * HEAD_DIM), D ** -0.5, 0.125)
    w_value = bell_draw(key_list[5], (D, KV_HEADS * HEAD_DIM), D ** -0.5, 0.125)
    w_out = bell_draw(key_list[6], (HEADS * HEAD_DIM, D), (HEADS * HEAD_DIM) ** -0.5, 0.1875)
    return dict(tokens=tokens, doc_lengths=doc_lengths, picked=picked, w_query=w_query, w_key=w_key, w_value=w_value, w_out=w_out)


def rotate(values_in, positions):
    half = values_in.shape[-1] // 2
    inverse = 10000.0 ** (-jnp.arange(half, dtype=jnp.float32) / half)
    angles = positions.astype(jnp.float32)[:, None] * inverse[None, :]
    cosine = jnp.cos(angles)[:, None, :]
    sine = jnp.sin(angles)[:, None, :]
    first = values_in[..., :half]
    second = values_in[..., half:]
    return jnp.concatenate([first * cosine - second * sine, second * cosine + first * sine], axis=-1)


def doc_of(positions, ends):
    return jnp.sum((positions[..., None] >= ends).astype(jnp.int32), axis=-1)


def one_group(tokens, doc_lengths, picked, w_query, w_key, w_value, w_out):
    seq = tokens.shape[0]
    positions = jnp.arange(seq, dtype=jnp.int32)
    ends = jnp.cumsum(doc_lengths).astype(jnp.int32)
    queries = rotate(jnp.dot(tokens, w_query, preferred_element_type=jnp.float32).reshape(seq, HEADS, HEAD_DIM), positions).astype(jnp.bfloat16)
    keys = rotate(jnp.dot(tokens, w_key, preferred_element_type=jnp.float32).reshape(seq, KV_HEADS, HEAD_DIM), positions).astype(jnp.bfloat16)
    values = jnp.dot(tokens, w_value, preferred_element_type=jnp.float32).astype(jnp.bfloat16).reshape(seq, KV_HEADS, HEAD_DIM)
    queries, keys, values = lax.optimization_barrier((queries, keys, values))
    group = HEADS // KV_HEADS
    offsets = jnp.arange(BLOCK, dtype=jnp.int32)

    def attend_block(index):
        start = (index * BLOCK).astype(jnp.int32)
        rows = lax.dynamic_slice_in_dim(queries, start, BLOCK, 0)
        query_pos = start + offsets
        slots = picked[index]
        key_pos = (jnp.maximum(slots, 0)[:, None] * BLOCK + offsets[None, :]).reshape(-1).astype(jnp.int32)
        block_keys = keys[key_pos].astype(jnp.float32)
        block_values = values[key_pos].astype(jnp.float32)
        filled = jnp.repeat(slots >= 0, BLOCK)
        live = filled[None, :] & (key_pos[None, :] <= query_pos[:, None]) & (doc_of(key_pos, ends)[None, :] == doc_of(query_pos, ends)[:, None])
        grouped = rows.astype(jnp.float32).reshape(BLOCK, KV_HEADS, group, HEAD_DIM)
        scores = jnp.einsum('qngd,knd->ngqk', grouped, block_keys) * (HEAD_DIM ** -0.5)
        scores = jnp.where(live[None, None], scores, -jnp.inf)
        highest = jnp.max(scores, axis=-1, keepdims=True)
        weights = jnp.exp(scores - highest)
        total = jnp.sum(weights, axis=-1)
        rounded = lax.optimization_barrier(weights.astype(jnp.bfloat16))
        summed = jnp.einsum('ngqk,knd->qngd', rounded.astype(jnp.float32), block_values)
        result = summed / jnp.transpose(total, (2, 0, 1))[..., None]
        return result.astype(jnp.bfloat16).reshape(BLOCK, HEADS * HEAD_DIM)

    attended = lax.map(attend_block, jnp.arange(seq // BLOCK, dtype=jnp.int32)).reshape(seq, HEADS * HEAD_DIM)
    return jnp.dot(attended, w_out, preferred_element_type=jnp.float32).astype(jnp.bfloat16)


def reference(tokens, doc_lengths, picked, w_query, w_key, w_value, w_out):
    def run(index):
        return one_group(tokens[index], doc_lengths[index], picked[index], w_query, w_key, w_value, w_out)

    return lax.map(run, jnp.arange(tokens.shape[0], dtype=jnp.int32))
```

```python
import functools

import jax
import jax.numpy as jnp
import numpy as np
from jax import lax
from jax.experimental import pallas as pl
from jax.experimental.pallas import tpu as pltpu
from jax.sharding import PartitionSpec as P

HEAD_DIM = 64
BLOCK = 32
LANES = 128
HOT = 2
MESH = pl.DeviceIdType.MESH
SCALE = float(HEAD_DIM ** -0.5 * np.log2(np.e))
F32 = jnp.float32
BF16 = jnp.bfloat16


def tables(rows, count):
    lane = np.arange(LANES)
    half = HEAD_DIM // 2
    inverse = (10000.0 ** (-(lane % half) / half)).astype(np.float32).astype(np.float64)
    sign = np.where(lane % HEAD_DIM < half, -1.0, 1.0)
    row = np.arange(rows)[:, None] * inverse
    start = (np.arange(count) * rows)[:, None] * inverse
    inner = np.stack([np.cos(row), np.sin(row) * sign]).astype(np.float32)
    outer = np.zeros((count, 8, LANES), np.float32)
    outer[:, 0] = np.cos(start)
    outer[:, 1] = np.sin(start) * sign
    return inner, outer


def iota(shape, axis):
    return lax.broadcasted_iota(jnp.int32, shape, axis)


def dot_t(a, b):
    return lax.dot_general(a, b, (((1,), (1,)), ((), ())), preferred_element_type=F32)


def dot(a, b):
    return jnp.dot(a, b, preferred_element_type=F32)


def kernel(
    n, tok_hbm, doc_hbm, pick_hbm, wq_hbm, wk_hbm, wv_hbm, wo_hbm, inner_hbm, outer_hbm, out_hbm,
    tok, doc, pick, wq, wk, wv, wo, inner, outer, names, names_in, kv_own, pack, hot_in,
    q_all, acc, top, att, att_in, partial, out, load_sem, name_s, name_r, hot_s, hot_r, att_s, att_r, out_sem,
):
    kv = lax.axis_index("kv")
    tp = lax.axis_index("tp")
    rows = tok.shape[0]
    blocks = rows // BLOCK
    heads = wq.shape[1] // HEAD_DIM
    wide = names.shape[1]
    mine = wo.shape[1]

    barrier = pltpu.get_barrier_semaphore()

    def greet(d, _):
        @pl.when(d != kv)
        def _():
            pl.semaphore_signal(barrier, inc=1, device_id={"kv": d}, device_id_type=MESH)
        return 0

    lax.fori_loop(0, n, greet, 0)
    pl.semaphore_signal(barrier, inc=1, device_id={"tp": 1 - tp}, device_id_type=MESH)

    pairs = [
        (pick_hbm.at[0], pick), (doc_hbm, doc), (tok_hbm.at[0], tok), (wk_hbm, wk), (wv_hbm, wv),
        (inner_hbm, inner), (outer_hbm.at[kv], outer), (wq_hbm, wq),
        (wo_hbm.at[pl.ds(tp * mine, mine)], wo.at[0]), (wo_hbm.at[pl.ds((1 - tp) * mine, mine)], wo.at[1]),
    ]
    loads = [pltpu.make_async_copy(a, b, load_sem.at[i]) for i, (a, b) in enumerate(pairs)]
    for load in loads:
        load.start()
    l_pick, l_doc, l_tok, l_wk, l_wv, l_in, l_out, l_wq, l_wo0, l_wo1 = loads

    l_pick.wait()
    slots = pick[...]
    block_ids = iota((blocks, wide), 1)
    hit = slots[:, 0:1] == block_ids
    for s in range(1, slots.shape[1]):
        hit = hit | (slots[:, s:s + 1] == block_ids)
    named_any = jnp.max(jnp.where(hit, 1.0, 0.0), axis=0, keepdims=True)
    names[...] = jnp.broadcast_to(named_any, names.shape)

    pl.semaphore_wait(barrier, n)

    def name_copy(d, source):
        return pltpu.make_async_remote_copy(
            src_ref=names, dst_ref=names_in.at[source], send_sem=name_s.at[d], recv_sem=name_r.at[source],
            device_id={"kv": d}, device_id_type=MESH)

    def name_send(d, _):
        name_copy(d, kv).start()
        return 0

    lax.fori_loop(0, kv, name_send, 0)

    def clear(d, _):
        hot_in[d] = jnp.zeros(hot_in.shape[1:], BF16)
        return 0

    lax.fori_loop(kv, n, clear, 0)

    l_in.wait()
    l_out.wait()
    cos_o, sin_o = outer[0:1, :], outer[1:2, :]
    cos_i, sin_i = inner[0], inner[1]
    cosine = cos_o * cos_i - sin_o * sin_i
    sine = sin_o * cos_i + cos_o * sin_i
    lane = iota((rows, LANES), 1)
    low = lane < HEAD_DIM
    first = lane % HEAD_DIM < HEAD_DIM // 2
    quarter = HEAD_DIM // 2

    def rotate(x):
        other = jnp.where(first, pltpu.roll(x, LANES - quarter, 1), pltpu.roll(x, quarter, 1))
        return x * cosine + other * sine

    def swap(x):
        return pltpu.roll(x, HEAD_DIM, 1)

    l_tok.wait()
    l_wk.wait()
    l_wv.wait()
    keys = rotate(dot(tok[...], wk[...]))
    values = dot(tok[...], wv[...])
    is_first = tp == 0
    keys = jnp.where(is_first, keys, swap(keys))
    values = jnp.where(is_first, swap(values), values)
    packed = jnp.where(low, keys, values).astype(BF16)
    kv_own[...] = packed

    def name_take(d, total):
        name_copy(d, d).wait_recv()
        return total + names_in[d]

    total = lax.fori_loop(kv + 1, n, name_take, jnp.zeros(names.shape, F32))
    flags = jnp.where(total > 0.0, 1.0, 0.0).astype(BF16)
    j = iota((wide, rows), 0) - kv * blocks
    col = iota((wide, rows), 1) // BLOCK
    here = dot(flags, jnp.where(j == col, 1.0, 0.0).astype(BF16))[0:1, :]
    rank = dot(flags, jnp.where((j >= 0) & (j < col), 1.0, 0.0).astype(BF16))[0:1, :]
    kept = HOT * BLOCK
    slot = iota((2 * kept, rows), 0) % kept
    own = iota((2 * kept, rows), 1)
    choose = (here > 0.5) & (rank == (slot // BLOCK).astype(F32)) & (own % BLOCK == slot % BLOCK)
    choose = jnp.where(choose, 1.0, 0.0).astype(BF16)
    label = (iota((16, rows), 1) // BLOCK + 1).astype(F32).astype(BF16)
    pack[0:kept, :] = dot(choose[0:kept], packed).astype(BF16)
    pack[kept:kept + 16, :] = dot_t(label, choose).astype(BF16)

    def hot_copy(d, source):
        return pltpu.make_async_remote_copy(
            src_ref=pack, dst_ref=hot_in.at[source], send_sem=hot_s.at[d], recv_sem=hot_r.at[source],
            device_id={"kv": d}, device_id_type=MESH)

    def hot_send(d, _):
        hot_copy(d, kv).start()
        return 0

    lax.fori_loop(kv + 1, n, hot_send, 0)

    l_wq.wait()
    queries = dot(tok[...], wq[...])
    for p in range(heads // 2):
        turned = rotate(queries[:, p * LANES:(p + 1) * LANES])
        q_all[2 * p * rows:(2 * p + 1) * rows, :] = jnp.where(low, turned, 0.0).astype(BF16)
        q_all[(2 * p + 1) * rows:(2 * p + 2) * rows, :] = jnp.where(low, swap(turned), 0.0).astype(BF16)

    l_doc.wait()
    q_pos = kv * rows + iota((rows, 1), 0)
    q_start = jnp.zeros((rows, 1), jnp.int32)
    end = jnp.int32(0)
    for i in range(doc.shape[1]):
        end = end + doc[0, i]
        q_start = jnp.where(q_pos >= end, end, q_start)

    def bias_of(key_block, key_pos):
        hits = slots[:, 0:1] == key_block
        for s in range(1, slots.shape[1]):
            hits = hits | (slots[:, s:s + 1] == key_block)
        allowed = jnp.where(hits, 0.0, -jnp.inf)
        parts = []
        for b in range(blocks):
            span = slice(b * BLOCK, (b + 1) * BLOCK)
            seen = (key_pos <= q_pos[span]) & (key_pos >= q_start[span])
            parts.append(jnp.where(seen, allowed[b:b + 1, :], -jnp.inf))
        return jnp.concatenate(parts, axis=0)

    def with_ones(block):
        return jnp.where(iota(block.shape, 1) < HEAD_DIM, jnp.ones((), BF16), block)

    local_col = iota((1, rows), 1)
    bias = bias_of(kv * blocks + local_col // BLOCK, kv * rows + local_col)
    both = jnp.concatenate([bias, bias], axis=0)
    ones_values = with_ones(packed)
    for p in range(heads // 2):
        span = slice(2 * p * rows, (2 * p + 2) * rows)
        scores = dot_t(q_all[span, :], packed) * SCALE + both
        highest = jnp.max(scores, axis=-1, keepdims=True)
        weights = jnp.exp2(scores - highest).astype(BF16)
        acc[span, :] = dot(weights, ones_values)
        top[span, :] = jnp.broadcast_to(highest, (2 * rows, LANES))

    def att_copy(h):
        return pltpu.make_async_remote_copy(
            src_ref=att.at[h], dst_ref=att_in.at[h], send_sem=att_s.at[h], recv_sem=att_r.at[h],
            device_id={"tp": 1 - tp}, device_id_type=MESH)

    def hot_wait(d, _):
        hot_copy(d, d).wait_recv()
        return 0

    lax.fori_loop(0, kv, hot_wait, 0)
    near = min(n, 8)
    width = att.shape[2]

    def group(g, last):
        start = g * near
        blocks_in = hot_in[pl.ds(start, near)]
        block = blocks_in[:, 0:kept, :].reshape(near * kept, LANES)
        upper = iota((1, LANES), 1) < kept
        ids = []
        for d in range(0, near, 2):
            even = hot_in[start + d, kept:kept + 16, :][0:1, :].astype(F32).astype(jnp.int32)
            odd = hot_in[start + d + 1, kept:kept + 16, :][0:1, :].astype(F32).astype(jnp.int32)
            even = jnp.where(even > 0, (start + d) * blocks + even - 1, -2)
            odd = jnp.where(odd > 0, (start + d + 1) * blocks + odd - 1, -2)
            ids.append(jnp.where(upper, even, odd))
        key_block = jnp.concatenate(ids, axis=1)
        key_pos = key_block * BLOCK + iota((1, near * kept), 1) % BLOCK
        bias = bias_of(key_block, key_pos)
        both = jnp.concatenate([bias, bias], axis=0)
        ones_values = with_ones(block)
        for p in range(heads // 2):
            span = slice(2 * p * rows, (2 * p + 2) * rows)
            scores = dot_t(q_all[span, :], block) * SCALE + both
            before = top[span, :]
            highest = jnp.maximum(before, jnp.max(scores, axis=-1, keepdims=True))
            weights = jnp.exp2(scores - highest[:, 0:1]).astype(BF16)
            summed = acc[span, :] * jnp.exp2(before - highest) + dot(weights, ones_values)
            if not last:
                acc[span, :] = summed
                top[span, :] = highest
                continue
            even, odd = summed[0:rows], summed[rows:]
            above = jnp.where(low, swap(even), odd)
            below = jnp.where(low, even, swap(odd))
            half, place = divmod(p * LANES, width)
            att[half, :, place:place + LANES] = (above / below).astype(BF16)
            if place + LANES == width:
                att_copy(half).start()

    if n > near:
        def step(g, _):
            group(g, False)
            return 0

        lax.fori_loop(0, n // near - 1, step, 0)
    group(n // near - 1, True)

    l_wo0.wait()
    halves = att.shape[0]
    columns = wo.shape[2]
    piece = columns // 4
    for c in range(4):
        cut = slice(c * piece, (c + 1) * piece)
        value = dot(att[0], wo[0, 0:width, cut])
        for h in range(1, halves):
            value += dot(att[h], wo[0, h * width:(h + 1) * width, cut])
        partial[:, cut] = value
    l_wo1.wait()
    for h in range(halves):
        att_copy(h).wait_recv()
    stores = []
    for c in range(4):
        cut = slice(c * piece, (c + 1) * piece)
        value = partial[:, cut]
        for h in range(halves):
            value += dot(att_in[h], wo[1, h * width:(h + 1) * width, cut])
        out[:, cut] = value.astype(BF16)
        store = pltpu.make_async_copy(out.at[:, cut], out_hbm.at[0, :, cut], out_sem.at[c])
        store.start()
        stores.append(store)
    for store in stores:
        store.wait()

    def name_done(d, _):
        name_copy(d, kv).wait_send()
        return 0

    def hot_done(d, _):
        hot_copy(d, kv).wait_send()
        return 0

    lax.fori_loop(0, kv, name_done, 0)
    lax.fori_loop(kv + 1, n, hot_done, 0)
    for h in range(halves):
        att_copy(h).wait_send()


def solution(mesh):
    n = mesh.shape["kv"]

    def shards(tokens, doc_lengths, picked, w_query, w_key, w_value, w_out):
        _, rows, d = tokens.shape
        blocks = rows // BLOCK
        wide = -(-n * blocks // LANES) * LANES
        q_cols = w_query.shape[1]
        heads = q_cols // HEAD_DIM
        columns = w_out.shape[1]
        inner, outer = tables(rows, n)
        width = q_cols // 2
        dma = pltpu.SemaphoreType.DMA
        payload = HOT * BLOCK + 16
        return pl.pallas_call(
            functools.partial(kernel, n),
            out_shape=jax.ShapeDtypeStruct((1, rows, columns), BF16),
            in_specs=[pl.BlockSpec(memory_space=pl.ANY)] * 9,
            out_specs=pl.BlockSpec(memory_space=pl.ANY),
            scratch_shapes=[
                pltpu.VMEM((rows, d), BF16),
                pltpu.SMEM(doc_lengths.shape, jnp.int32),
                pltpu.VMEM(picked.shape[1:], jnp.int32),
                pltpu.VMEM(w_query.shape, BF16),
                pltpu.VMEM(w_key.shape, BF16),
                pltpu.VMEM(w_value.shape, BF16),
                pltpu.VMEM((2, w_out.shape[0] // 2, columns), BF16),
                pltpu.VMEM(inner.shape, F32),
                pltpu.VMEM(outer.shape[1:], F32),
                pltpu.VMEM((8, wide), F32),
                pltpu.VMEM((n, 8, wide), F32),
                pltpu.VMEM((rows, LANES), BF16),
                pltpu.VMEM((payload, LANES), BF16),
                pltpu.VMEM((n, payload, LANES), BF16),
                pltpu.VMEM((heads * rows, LANES), BF16),
                pltpu.VMEM((heads * rows, LANES), F32),
                pltpu.VMEM((heads * rows, LANES), F32),
                pltpu.VMEM((2, rows, width), BF16),
                pltpu.VMEM((2, rows, width), BF16),
                pltpu.VMEM((rows, columns), F32),
                pltpu.VMEM((rows, columns), BF16),
                dma((10,)), dma((n,)), dma((n,)), dma((n,)), dma((n,)), dma((2,)), dma((2,)), dma((4,)),
            ],
            compiler_params=pltpu.CompilerParams(
                collective_id=0, has_side_effects=True, vmem_limit_bytes=56 * 1024 * 1024
            ),
        )(tokens, doc_lengths, picked, w_query, w_key, w_value, w_out, inner, outer)

    placed = (P("dp", "kv", None), P("dp", None), P("dp", "kv", None), P(None, "tp"), P(), P(), P())
    return jax.shard_map(
        shards, mesh=mesh, in_specs=placed, out_specs=P("dp", "kv", None), check_vma=False
    )
```

```python
import functools

import jax
import jax.numpy as jnp
import numpy as np
from jax import lax
from jax.experimental import pallas as pl
from jax.experimental.pallas import tpu as pltpu
from jax.sharding import PartitionSpec as P

HEAD_DIM = 64
BLOCK = 32
LANES = 128
HOT = 2
MESH = pl.DeviceIdType.MESH
SCALE = float(HEAD_DIM ** -0.5 * np.log2(np.e))
F32 = jnp.float32
BF16 = jnp.bfloat16


def tables(rows, count):
    lane = np.arange(LANES)
    half = HEAD_DIM // 2
    inverse = (10000.0 ** (-(lane % half) / half)).astype(np.float32).astype(np.float64)
    sign = np.where(lane % HEAD_DIM < half, -1.0, 1.0)
    row = np.arange(rows)[:, None] * inverse
    start = (np.arange(count) * rows)[:, None] * inverse
    inner = np.stack([np.cos(row), np.sin(row) * sign]).astype(np.float32)
    outer = np.zeros((count, 8, LANES), np.float32)
    outer[:, 0] = np.cos(start)
    outer[:, 1] = np.sin(start) * sign
    return inner, outer


def iota(shape, axis):
    return lax.broadcasted_iota(jnp.int32, shape, axis)


def dot_t(a, b):
    return lax.dot_general(a, b, (((1,), (1,)), ((), ())), preferred_element_type=F32)


def dot(a, b):
    return jnp.dot(a, b, preferred_element_type=F32)


def kernel(
    n, tok_hbm, doc_hbm, pick_hbm, wq_hbm, wk_hbm, wv_hbm, wo_hbm, inner_hbm, outer_hbm, out,
    tok, doc, pick, wq, wkv, wo, inner, outer, names, names_in, kv_own, pack, hot_in,
    q_all, acc, top, att, att_in, partial, load_sem, name_s, name_r, hot_s, hot_r, att_s, att_r,
):
    kv = lax.axis_index("kv")
    tp = lax.axis_index("tp")
    rows = tok.shape[0]
    blocks = rows // BLOCK
    heads = wq.shape[1] // HEAD_DIM
    wide = names.shape[1]
    mine = wo.shape[1]

    barrier = pltpu.get_barrier_semaphore()

    def greet(d, _):
        @pl.when(d != kv)
        def _():
            pl.semaphore_signal(barrier, inc=1, device_id={"kv": d}, device_id_type=MESH)
        return 0

    lax.fori_loop(0, n, greet, 0)
    pl.semaphore_signal(barrier, inc=1, device_id={"tp": 1 - tp}, device_id_type=MESH)

    pairs = [
        (pick_hbm, pick), (doc_hbm, doc), (tok_hbm.at[0], tok), (wk_hbm, wkv.at[:, 0:LANES]), (wv_hbm, wkv.at[:, LANES:]),
        (inner_hbm, inner), (outer_hbm.at[kv], outer), (wq_hbm, wq),
        (wo_hbm.at[pl.ds(tp * mine, mine)], wo.at[0]), (wo_hbm.at[pl.ds((1 - tp) * mine, mine)], wo.at[1]),
    ]
    loads = [pltpu.make_async_copy(a, b, load_sem.at[i]) for i, (a, b) in enumerate(pairs)]
    for load in loads:
        load.start()
    l_pick, l_doc, l_tok, l_wk, l_wv, l_in, l_out, l_wq, l_wo0, l_wo1 = loads

    l_pick.wait()
    slots = jnp.concatenate([pick[b] for b in range(blocks)], axis=0)
    block_ids = iota((blocks, wide), 1)
    hit = slots[:, 0:1] == block_ids
    for s in range(1, slots.shape[1]):
        hit = hit | (slots[:, s:s + 1] == block_ids)
    named_any = jnp.max(jnp.where(hit, 1.0, 0.0), axis=0, keepdims=True)
    names[...] = jnp.broadcast_to(named_any, names.shape)

    pl.semaphore_wait(barrier, n)

    def name_copy(d, source):
        return pltpu.make_async_remote_copy(
            src_ref=names, dst_ref=names_in.at[source], send_sem=name_s.at[d], recv_sem=name_r.at[source],
            device_id={"kv": d}, device_id_type=MESH)

    def name_send(d, _):
        name_copy(d, kv).start()
        return 0

    lax.fori_loop(0, kv, name_send, 0)

    def clear(d, _):
        hot_in[d] = jnp.zeros(hot_in.shape[1:], BF16)
        return 0

    lax.fori_loop(kv, n, clear, 0)

    l_in.wait()
    l_out.wait()
    cos_o, sin_o = outer[0:1, :], outer[1:2, :]
    cos_i, sin_i = inner[0], inner[1]
    cosine = cos_o * cos_i - sin_o * sin_i
    sine = sin_o * cos_i + cos_o * sin_i
    lane = iota((rows, LANES), 1)
    low = lane < HEAD_DIM
    first = lane % HEAD_DIM < HEAD_DIM // 2
    quarter = HEAD_DIM // 2

    def rotate(x):
        other = jnp.where(first, pltpu.roll(x, LANES - quarter, 1), pltpu.roll(x, quarter, 1))
        return x * cosine + other * sine

    def swap(x):
        return pltpu.roll(x, HEAD_DIM, 1)

    l_tok.wait()
    l_wk.wait()
    l_wv.wait()
    both = dot(tok[...], wkv[...])
    keys = rotate(both[:, 0:LANES])
    values = both[:, LANES:]
    is_first = tp == 0
    keys = jnp.where(is_first, keys, swap(keys))
    values = jnp.where(is_first, swap(values), values)
    packed = jnp.where(low, keys, values).astype(BF16)
    kv_own[...] = packed

    def name_take(d, total):
        name_copy(d, d).wait_recv()
        return total + names_in[d]

    total = lax.fori_loop(kv + 1, n, name_take, jnp.zeros(names.shape, F32))
    flags = jnp.where(total > 0.0, 1.0, 0.0).astype(BF16)
    j = iota((wide, rows), 0) - kv * blocks
    col = iota((wide, rows), 1) // BLOCK
    here = dot(flags, jnp.where(j == col, 1.0, 0.0).astype(BF16))[0:1, :]
    rank = dot(flags, jnp.where((j >= 0) & (j < col), 1.0, 0.0).astype(BF16))[0:1, :]
    kept = HOT * BLOCK
    slot = iota((2 * kept, rows), 0) % kept
    own = iota((2 * kept, rows), 1)
    choose = (here > 0.5) & (rank == (slot // BLOCK).astype(F32)) & (own % BLOCK == slot % BLOCK)
    choose = jnp.where(choose, 1.0, 0.0).astype(BF16)
    label = (iota((16, rows), 1) // BLOCK + 1).astype(F32).astype(BF16)
    pack[0:kept, :] = dot(choose[0:kept], packed).astype(BF16)
    pack[kept:kept + 16, :] = dot_t(label, choose).astype(BF16)

    def hot_copy(d, source):
        return pltpu.make_async_remote_copy(
            src_ref=pack, dst_ref=hot_in.at[source], send_sem=hot_s.at[d], recv_sem=hot_r.at[source],
            device_id={"kv": d}, device_id_type=MESH)

    def hot_send(d, _):
        hot_copy(d, kv).start()
        return 0

    lax.fori_loop(kv + 1, n, hot_send, 0)

    l_wq.wait()
    queries = dot(tok[...], wq[...])
    for p in range(heads // 2):
        turned = rotate(queries[:, p * LANES:(p + 1) * LANES])
        q_all[2 * p * rows:(2 * p + 1) * rows, :] = jnp.where(low, turned, 0.0).astype(BF16)
        q_all[(2 * p + 1) * rows:(2 * p + 2) * rows, :] = jnp.where(low, swap(turned), 0.0).astype(BF16)

    l_doc.wait()
    q_pos = kv * rows + iota((rows, 1), 0)
    q_start = jnp.zeros((rows, 1), jnp.int32)
    end = jnp.int32(0)
    for i in range(doc.shape[1]):
        end = end + doc[0, i]
        q_start = jnp.where(q_pos >= end, end, q_start)

    def bias_of(key_block, key_pos):
        hits = slots[:, 0:1] == key_block
        for s in range(1, slots.shape[1]):
            hits = hits | (slots[:, s:s + 1] == key_block)
        allowed = jnp.where(hits, 0.0, -jnp.inf)
        parts = []
        for b in range(blocks):
            span = slice(b * BLOCK, (b + 1) * BLOCK)
            seen = (key_pos <= q_pos[span]) & (key_pos >= q_start[span])
            parts.append(jnp.where(seen, allowed[b:b + 1, :], -jnp.inf))
        return jnp.concatenate(parts, axis=0)

    def with_ones(block):
        return jnp.where(iota(block.shape, 1) < HEAD_DIM, jnp.ones((), BF16), block)

    local_col = iota((1, rows), 1)
    bias = bias_of(kv * blocks + local_col // BLOCK, kv * rows + local_col)
    both = jnp.concatenate([bias, bias], axis=0)
    ones_values = with_ones(packed)
    for p in range(heads // 2):
        span = slice(2 * p * rows, (2 * p + 2) * rows)
        scores = dot_t(q_all[span, :], packed) * SCALE + both
        highest = jnp.max(scores, axis=-1, keepdims=True)
        weights = jnp.exp2(scores - highest).astype(BF16)
        acc[span, :] = dot(weights, ones_values)
        top[span, :] = jnp.broadcast_to(highest, (2 * rows, LANES))

    def att_copy(h):
        return pltpu.make_async_remote_copy(
            src_ref=att.at[h], dst_ref=att_in.at[h], send_sem=att_s.at[h], recv_sem=att_r.at[h],
            device_id={"tp": 1 - tp}, device_id_type=MESH)

    def hot_wait(d, _):
        hot_copy(d, d).wait_recv()
        return 0

    lax.fori_loop(0, kv, hot_wait, 0)
    near = min(n, 8)
    width = att.shape[2]

    def group(g, last):
        start = g * near
        blocks_in = hot_in[pl.ds(start, near)]
        block = blocks_in[:, 0:kept, :].reshape(near * kept, LANES)
        upper = iota((1, LANES), 1) < kept
        ids = []
        for d in range(0, near, 2):
            even = hot_in[start + d, kept:kept + 16, :][0:1, :].astype(F32).astype(jnp.int32)
            odd = hot_in[start + d + 1, kept:kept + 16, :][0:1, :].astype(F32).astype(jnp.int32)
            even = jnp.where(even > 0, (start + d) * blocks + even - 1, -2)
            odd = jnp.where(odd > 0, (start + d + 1) * blocks + odd - 1, -2)
            ids.append(jnp.where(upper, even, odd))
        key_block = jnp.concatenate(ids, axis=1)
        key_pos = key_block * BLOCK + iota((1, near * kept), 1) % BLOCK
        bias = bias_of(key_block, key_pos)
        both = jnp.concatenate([bias, bias], axis=0)
        ones_values = with_ones(block)
        for p in range(heads // 2):
            span = slice(2 * p * rows, (2 * p + 2) * rows)
            scores = dot_t(q_all[span, :], block) * SCALE + both
            before = top[span, :]
            highest = jnp.maximum(before, jnp.max(scores, axis=-1, keepdims=True))
            weights = jnp.exp2(scores - highest[:, 0:1]).astype(BF16)
            summed = acc[span, :] * jnp.exp2(before - highest) + dot(weights, ones_values)
            if not last:
                acc[span, :] = summed
                top[span, :] = highest
                continue
            even, odd = summed[0:rows], summed[rows:]
            above = jnp.where(low, swap(even), odd)
            below = jnp.where(low, even, swap(odd))
            half, place = divmod(p * LANES, width)
            att[half, :, place:place + LANES] = (above / below).astype(BF16)
            if place + LANES == width:
                att_copy(half).start()

    if n > near:
        def step(g, _):
            group(g, False)
            return 0

        lax.fori_loop(0, n // near - 1, step, 0)
    group(n // near - 1, True)

    l_wo0.wait()
    halves = att.shape[0]
    columns = wo.shape[2]
    piece = columns // 4
    for c in range(4):
        cut = slice(c * piece, (c + 1) * piece)
        value = dot(att[0], wo[0, 0:width, cut])
        for h in range(1, halves):
            value += dot(att[h], wo[0, h * width:(h + 1) * width, cut])
        partial[:, cut] = value
    l_wo1.wait()
    for h in range(halves):
        att_copy(h).wait_recv()
    for c in range(4):
        cut = slice(c * piece, (c + 1) * piece)
        value = partial[:, cut]
        for h in range(halves):
            value += dot(att_in[h], wo[1, h * width:(h + 1) * width, cut])
        out[0, :, cut] = value.astype(BF16)

    def name_done(d, _):
        name_copy(d, kv).wait_send()
        return 0

    def hot_done(d, _):
        hot_copy(d, kv).wait_send()
        return 0

    lax.fori_loop(0, kv, name_done, 0)
    lax.fori_loop(kv + 1, n, hot_done, 0)
    for h in range(halves):
        att_copy(h).wait_send()


def solution(mesh):
    n = mesh.shape["kv"]

    def shards(tokens, doc_lengths, picked, w_query, w_key, w_value, w_out):
        _, rows, d = tokens.shape
        blocks = rows // BLOCK
        wide = -(-n * blocks // LANES) * LANES
        q_cols = w_query.shape[1]
        heads = q_cols // HEAD_DIM
        columns = w_out.shape[1]
        inner, outer = tables(rows, n)
        width = q_cols // 2
        dma = pltpu.SemaphoreType.DMA
        payload = HOT * BLOCK + 16
        operands = (tokens, doc_lengths, jnp.transpose(picked, (1, 0, 2)), w_query, w_key, w_value, w_out, inner, outer)
        operands = [pltpu.with_memory_space_constraint(jnp.asarray(x), pltpu.HBM) for x in operands]
        return pl.pallas_call(
            functools.partial(kernel, n),
            out_shape=jax.ShapeDtypeStruct((1, rows, columns), BF16),
            in_specs=[pl.BlockSpec(memory_space=pltpu.HBM)] * 9,
            out_specs=pl.BlockSpec(memory_space=pltpu.VMEM),
            scratch_shapes=[
                pltpu.VMEM((rows, d), BF16),
                pltpu.SMEM(doc_lengths.shape, jnp.int32),
                pltpu.VMEM((blocks, 1, picked.shape[2]), jnp.int32),
                pltpu.VMEM(w_query.shape, BF16),
                pltpu.VMEM((d, 2 * LANES), BF16),
                pltpu.VMEM((2, w_out.shape[0] // 2, columns), BF16),
                pltpu.VMEM(inner.shape, F32),
                pltpu.VMEM(outer.shape[1:], F32),
                pltpu.VMEM((8, wide), F32),
                pltpu.VMEM((n, 8, wide), F32),
                pltpu.VMEM((rows, LANES), BF16),
                pltpu.VMEM((payload, LANES), BF16),
                pltpu.VMEM((n, payload, LANES), BF16),
                pltpu.VMEM((heads * rows, LANES), BF16),
                pltpu.VMEM((heads * rows, LANES), F32),
                pltpu.VMEM((heads * rows, LANES), F32),
                pltpu.VMEM((2, rows, width), BF16),
                pltpu.VMEM((2, rows, width), BF16),
                pltpu.VMEM((rows, columns), F32),
                dma((10,)), dma((n,)), dma((n,)), dma((n,)), dma((n,)), dma((2,)), dma((2,)),
            ],
            compiler_params=pltpu.CompilerParams(
                collective_id=0, has_side_effects=True, vmem_limit_bytes=24 * 1024 * 1024
            ),
        )(*operands)

    placed = (P("dp", "kv", None), P("dp", None), P("dp", "kv", None), P(None, "tp"), P(), P(), P())
    return jax.shard_map(
        shards, mesh=mesh, in_specs=placed, out_specs=P("dp", "kv", None), check_vma=False
    )
```

```python
import functools
import math

import jax
import jax.numpy as jnp
import numpy as np
from jax import lax
from jax.experimental import pallas as pl
from jax.experimental.pallas import tpu as pltpu
from jax.sharding import PartitionSpec as P

HEAD_DIM = 64
BLOCK = 32
LANES = 128
HOT = 2
MESH = pl.DeviceIdType.MESH
SCALE = float(HEAD_DIM ** -0.5 * np.log2(np.e))
F32 = jnp.float32
BF16 = jnp.bfloat16


def tables(rows, count):
    lane = np.arange(LANES)
    half = HEAD_DIM // 2
    inverse = (10000.0 ** (-(lane % half) / half)).astype(np.float32).astype(np.float64)
    sign = np.where(lane % HEAD_DIM < half, -1.0, 1.0)
    row = np.arange(rows)[:, None] * inverse
    start = (np.arange(count) * rows)[:, None] * inverse
    inner = np.stack([np.cos(row), np.sin(row) * sign]).astype(np.float32)
    outer = np.zeros((count, 8, LANES), np.float32)
    outer[:, 0] = np.cos(start)
    outer[:, 1] = np.sin(start) * sign
    return inner, outer


def iota(shape, axis):
    return lax.broadcasted_iota(jnp.int32, shape, axis)


def dot_t(a, b):
    return lax.dot_general(a, b, (((1,), (1,)), ((), ())), preferred_element_type=F32)


def dot(a, b):
    return jnp.dot(a, b, preferred_element_type=F32)


def kernel(
    n, reach, tok_hbm, doc_hbm, pick_hbm, wq_hbm, wk_hbm, wv_hbm, wo_hbm, inner_hbm, outer_hbm, out,
    tok, doc, pick, wq, wkv, wo, inner, outer, names, names_in, kv_own, pack, hot_in, ids, ids_in,
    q_all, acc, top, att, att_in, partial, load_sem, name_s, name_r, hot_s, hot_r, ids_s, ids_r, att_s, att_r,
):
    kv = lax.axis_index("kv")
    tp = lax.axis_index("tp")
    rows = tok.shape[0]
    blocks = rows // BLOCK
    heads = wq.shape[1] // HEAD_DIM
    wide = names.shape[1]
    mine = wo.shape[1]

    barrier = pltpu.get_barrier_semaphore()

    before = jnp.minimum(kv, reach)
    after = jnp.minimum(n - 1 - kv, reach)

    def greet(d, _):
        @pl.when(d != kv)
        def _():
            pl.semaphore_signal(barrier, inc=1, device_id={"kv": d}, device_id_type=MESH)
        return 0

    lax.fori_loop(kv - before, kv + after + 1, greet, 0)
    pl.semaphore_signal(barrier, inc=1, device_id={"tp": 1 - tp}, device_id_type=MESH)

    pairs = [
        (pick_hbm, pick), (doc_hbm, doc), (tok_hbm.at[0], tok), (wk_hbm, wkv.at[:, 0:LANES]), (wv_hbm, wkv.at[:, LANES:]),
        (inner_hbm, inner), (outer_hbm.at[kv], outer), (wq_hbm, wq),
        (wo_hbm.at[pl.ds(tp * mine, mine)], wo.at[0]), (wo_hbm.at[pl.ds((1 - tp) * mine, mine)], wo.at[1]),
    ]
    loads = [pltpu.make_async_copy(a, b, load_sem.at[i]) for i, (a, b) in enumerate(pairs)]
    for load in loads:
        load.start()
    l_pick, l_doc, l_tok, l_wk, l_wv, l_in, l_out, l_wq, l_wo0, l_wo1 = loads

    l_pick.wait()
    slots = jnp.concatenate([pick[b] for b in range(blocks)], axis=0)
    block_ids = iota((blocks, wide), 1)
    hit = slots[:, 0:1] == block_ids
    for s in range(1, slots.shape[1]):
        hit = hit | (slots[:, s:s + 1] == block_ids)
    named_any = jnp.max(jnp.where(hit, 1.0, 0.0), axis=0, keepdims=True)
    names[...] = jnp.broadcast_to(named_any, names.shape)

    pl.semaphore_wait(barrier, before + after + 1)

    def name_copy(i):
        return pltpu.make_async_remote_copy(
            src_ref=names, dst_ref=names_in.at[i], send_sem=name_s.at[i], recv_sem=name_r.at[i],
            device_id={"kv": kv - 1 - i}, device_id_type=MESH)

    def name_send(i, _):
        name_copy(i).start()
        return 0

    lax.fori_loop(0, before, name_send, 0)

    def clear(i, _):
        hot_in[i] = jnp.zeros(hot_in.shape[1:], BF16)
        ids_in[i] = jnp.zeros(ids_in.shape[1:], F32)
        return 0

    lax.fori_loop(before, reach, clear, 0)

    l_in.wait()
    l_out.wait()
    cos_o, sin_o = outer[0:1, :], outer[1:2, :]
    cos_i, sin_i = inner[0], inner[1]
    cosine = cos_o * cos_i - sin_o * sin_i
    sine = sin_o * cos_i + cos_o * sin_i
    lane = iota((rows, LANES), 1)
    low = lane < HEAD_DIM
    first = lane % HEAD_DIM < HEAD_DIM // 2
    quarter = HEAD_DIM // 2

    def rotate(x):
        other = jnp.where(first, pltpu.roll(x, LANES - quarter, 1), pltpu.roll(x, quarter, 1))
        return x * cosine + other * sine

    def swap(x):
        return pltpu.roll(x, HEAD_DIM, 1)

    l_tok.wait()
    l_wk.wait()
    l_wv.wait()
    both = dot(tok[...], wkv[...])
    keys = rotate(both[:, 0:LANES])
    values = both[:, LANES:]
    is_first = tp == 0
    keys = jnp.where(is_first, keys, swap(keys))
    values = jnp.where(is_first, swap(values), values)
    packed = jnp.where(low, keys, values).astype(BF16)
    kv_own[...] = packed

    l_wq.wait()
    queries = dot(tok[...], wq[...])
    for p in range(heads // 2):
        turned = rotate(queries[:, p * LANES:(p + 1) * LANES])
        q_all[2 * p * rows:(2 * p + 1) * rows, :] = jnp.where(low, turned, 0.0).astype(BF16)
        q_all[(2 * p + 1) * rows:(2 * p + 2) * rows, :] = jnp.where(low, swap(turned), 0.0).astype(BF16)

    def name_take(i, total):
        name_copy(i).wait_recv()
        return total + names_in[i]

    total = lax.fori_loop(0, after, name_take, jnp.zeros(names.shape, F32))
    flags = jnp.broadcast_to(jnp.where(total > 0.0, 1.0, 0.0), (8, wide)).astype(BF16)
    j = iota((wide, rows), 0) - kv * blocks
    col = iota((wide, rows), 1) // BLOCK
    here = dot(flags, jnp.where(j == col, 1.0, 0.0).astype(BF16))[0:1, :]
    rank = dot(flags, jnp.where((j >= 0) & (j < col), 1.0, 0.0).astype(BF16))[0:1, :]
    kept = HOT * BLOCK
    slot = iota((2 * kept, rows), 0) % kept
    own = iota((2 * kept, rows), 1)
    choose = (here > 0.5) & (rank == (slot // BLOCK).astype(F32)) & (own % BLOCK == slot % BLOCK)
    choose = jnp.where(choose, 1.0, 0.0).astype(BF16)
    label = (iota((16, rows), 1) // BLOCK + 1).astype(F32).astype(BF16)
    pack[...] = dot(choose[0:kept], packed).astype(BF16)
    ids[...] = dot_t(label, choose)[0:1, :]

    def hot_copy(i):
        return pltpu.make_async_remote_copy(
            src_ref=pack, dst_ref=hot_in.at[i], send_sem=hot_s.at[i], recv_sem=hot_r.at[i],
            device_id={"kv": kv + 1 + i}, device_id_type=MESH)

    def ids_copy(i):
        return pltpu.make_async_remote_copy(
            src_ref=ids, dst_ref=ids_in.at[i], send_sem=ids_s.at[i], recv_sem=ids_r.at[i],
            device_id={"kv": kv + 1 + i}, device_id_type=MESH)

    def hot_send(i, _):
        ids_copy(i).start()
        hot_copy(i).start()
        return 0

    lax.fori_loop(0, after, hot_send, 0)

    l_doc.wait()
    q_pos = kv * rows + iota((rows, 1), 0)
    q_start = jnp.zeros((rows, 1), jnp.int32)
    end = jnp.int32(0)
    for i in range(doc.shape[1]):
        end = end + doc[0, i]
        q_start = jnp.where(q_pos >= end, end, q_start)

    def bias_of(key_block, key_pos):
        hits = slots[:, 0:1] == key_block
        for s in range(1, slots.shape[1]):
            hits = hits | (slots[:, s:s + 1] == key_block)
        allowed = jnp.where(hits, 0.0, -jnp.inf)
        parts = []
        for b in range(blocks):
            span = slice(b * BLOCK, (b + 1) * BLOCK)
            seen = (key_pos <= q_pos[span]) & (key_pos >= q_start[span])
            parts.append(jnp.where(seen, allowed[b:b + 1, :], -jnp.inf))
        return jnp.concatenate(parts, axis=0)

    def with_ones(block):
        return jnp.where(iota(block.shape, 1) < HEAD_DIM, jnp.ones((), BF16), block)

    local_col = iota((1, rows), 1)
    bias = bias_of(kv * blocks + local_col // BLOCK, kv * rows + local_col)
    both = jnp.concatenate([bias, bias], axis=0)
    ones_values = with_ones(packed)
    for p in range(heads // 2):
        span = slice(2 * p * rows, (2 * p + 2) * rows)
        scores = dot_t(q_all[span, :], packed) * SCALE + both
        highest = jnp.max(scores, axis=-1, keepdims=True)
        weights = jnp.exp2(scores - highest).astype(BF16)
        acc[span, :] = dot(weights, ones_values)
        top[span, :] = jnp.broadcast_to(highest, (2 * rows, LANES))

    def att_copy(h):
        return pltpu.make_async_remote_copy(
            src_ref=att.at[h], dst_ref=att_in.at[h], send_sem=att_s.at[h], recv_sem=att_r.at[h],
            device_id={"tp": 1 - tp}, device_id_type=MESH)

    def hot_wait(i, _):
        ids_copy(i).wait_recv()
        hot_copy(i).wait_recv()
        return 0

    lax.fori_loop(0, before, hot_wait, 0)
    near = math.gcd(reach, 8)
    width = att.shape[2]

    def group(g, last):
        start = g * near
        block = hot_in[pl.ds(start, near)].reshape(near * kept, LANES)
        upper = iota((1, LANES), 1) < kept
        found = []
        for i in range(0, near, 2):
            base = (kv - 1 - start - i) * blocks - 1
            even = ids_in[start + i].astype(jnp.int32)
            odd = ids_in[start + i + 1].astype(jnp.int32)
            even = jnp.where(even > 0, base + even, -2)
            odd = jnp.where(odd > 0, base - blocks + odd, -2)
            found.append(jnp.where(upper, even, odd))
        key_block = jnp.concatenate(found, axis=1)
        key_pos = key_block * BLOCK + iota((1, near * kept), 1) % BLOCK
        bias = bias_of(key_block, key_pos)
        both = jnp.concatenate([bias, bias], axis=0)
        ones_values = with_ones(block)
        for p in range(heads // 2):
            span = slice(2 * p * rows, (2 * p + 2) * rows)
            scores = dot_t(q_all[span, :], block) * SCALE + both
            before = top[span, :]
            highest = jnp.maximum(before, jnp.max(scores, axis=-1, keepdims=True))
            weights = jnp.exp2(scores - highest[:, 0:1]).astype(BF16)
            summed = acc[span, :] * jnp.exp2(before - highest) + dot(weights, ones_values)
            if not last:
                acc[span, :] = summed
                top[span, :] = highest
                continue
            even, odd = summed[0:rows], summed[rows:]
            above = jnp.where(low, swap(even), odd)
            below = jnp.where(low, even, swap(odd))
            half, place = divmod(p * LANES, width)
            att[half, :, place:place + LANES] = (above / below).astype(BF16)
            if place + LANES == width:
                att_copy(half).start()

    if reach > near:
        def step(g, _):
            group(g, False)
            return 0

        lax.fori_loop(0, reach // near - 1, step, 0)
    group(reach // near - 1, True)

    l_wo0.wait()
    halves = att.shape[0]
    columns = wo.shape[2]
    piece = columns // 4
    for c in range(4):
        cut = slice(c * piece, (c + 1) * piece)
        value = dot(att[0], wo[0, 0:width, cut])
        for h in range(1, halves):
            value += dot(att[h], wo[0, h * width:(h + 1) * width, cut])
        partial[:, cut] = value
    l_wo1.wait()
    for h in range(halves):
        att_copy(h).wait_recv()
    for c in range(4):
        cut = slice(c * piece, (c + 1) * piece)
        value = partial[:, cut]
        for h in range(halves):
            value += dot(att_in[h], wo[1, h * width:(h + 1) * width, cut])
        out[0, :, cut] = value.astype(BF16)

    def name_done(i, _):
        name_copy(i).wait_send()
        return 0

    def hot_done(i, _):
        ids_copy(i).wait_send()
        hot_copy(i).wait_send()
        return 0

    lax.fori_loop(0, before, name_done, 0)
    lax.fori_loop(0, after, hot_done, 0)
    for h in range(halves):
        att_copy(h).wait_send()


def solution(mesh):
    n = mesh.shape["kv"]

    def shards(tokens, doc_lengths, picked, w_query, w_key, w_value, w_out):
        _, rows, d = tokens.shape
        blocks = rows // BLOCK
        wide = -(-n * blocks // LANES) * LANES
        q_cols = w_query.shape[1]
        heads = q_cols // HEAD_DIM
        columns = w_out.shape[1]
        inner, outer = tables(rows, n)
        width = q_cols // 2
        dma = pltpu.SemaphoreType.DMA
        payload = HOT * BLOCK
        reach = min(n, (n * rows // 2 + rows - 2) // rows)
        reach += reach % 2
        operands = (tokens, doc_lengths, jnp.transpose(picked, (1, 0, 2)), w_query, w_key, w_value, w_out, inner, outer)
        operands = [pltpu.with_memory_space_constraint(jnp.asarray(x), pltpu.HBM) for x in operands]
        return pl.pallas_call(
            functools.partial(kernel, n, reach),
            out_shape=jax.ShapeDtypeStruct((1, rows, columns), BF16),
            in_specs=[pl.BlockSpec(memory_space=pltpu.HBM)] * 9,
            out_specs=pl.BlockSpec(memory_space=pltpu.VMEM),
            scratch_shapes=[
                pltpu.VMEM((rows, d), BF16),
                pltpu.SMEM(doc_lengths.shape, jnp.int32),
                pltpu.VMEM((blocks, 1, picked.shape[2]), jnp.int32),
                pltpu.VMEM(w_query.shape, BF16),
                pltpu.VMEM((d, 2 * LANES), BF16),
                pltpu.VMEM((2, w_out.shape[0] // 2, columns), BF16),
                pltpu.VMEM(inner.shape, F32),
                pltpu.VMEM(outer.shape[1:], F32),
                pltpu.VMEM((1, wide), F32),
                pltpu.VMEM((reach, 1, wide), F32),
                pltpu.VMEM((rows, LANES), BF16),
                pltpu.VMEM((payload, LANES), BF16),
                pltpu.VMEM((reach, payload, LANES), BF16),
                pltpu.VMEM((1, LANES), F32),
                pltpu.VMEM((reach, 1, LANES), F32),
                pltpu.VMEM((heads * rows, LANES), BF16),
                pltpu.VMEM((heads * rows, LANES), F32),
                pltpu.VMEM((heads * rows, LANES), F32),
                pltpu.VMEM((2, rows, width), BF16),
                pltpu.VMEM((2, rows, width), BF16),
                pltpu.VMEM((rows, columns), F32),
                dma((10,)), *[dma((reach,))] * 6, dma((2,)), dma((2,)),
            ],
            compiler_params=pltpu.CompilerParams(
                collective_id=0, has_side_effects=True, vmem_limit_bytes=24 * 1024 * 1024
            ),
        )(*operands)

    placed = (P("dp", "kv", None), P("dp", None), P("dp", "kv", None), P(None, "tp"), P(), P(), P())
    return jax.shard_map(
        shards, mesh=mesh, in_specs=placed, out_specs=P("dp", "kv", None), check_vma=False
    )
```

```python
import functools
import math

import jax
import jax.numpy as jnp
import numpy as np
from jax import lax
from jax.experimental import pallas as pl
from jax.experimental.pallas import tpu as pltpu
from jax.sharding import PartitionSpec as P

HEAD_DIM = 64
BLOCK = 32
LANES = 128
HOT = 2
MESH = pl.DeviceIdType.MESH
SCALE = float(HEAD_DIM ** -0.5 * np.log2(np.e))
F32 = jnp.float32
BF16 = jnp.bfloat16


def tables(rows, count):
    lane = np.arange(LANES)
    half = HEAD_DIM // 2
    inverse = (10000.0 ** (-(lane % half) / half)).astype(np.float32).astype(np.float64)
    sign = np.where(lane % HEAD_DIM < half, -1.0, 1.0)
    row = np.arange(rows)[:, None] * inverse
    start = (np.arange(count) * rows)[:, None] * inverse
    inner = np.stack([np.cos(row), np.sin(row) * sign]).astype(np.float32)
    outer = np.zeros((count, 8, LANES), np.float32)
    outer[:, 0] = np.cos(start)
    outer[:, 1] = np.sin(start) * sign
    return inner, outer


def iota(shape, axis):
    return lax.broadcasted_iota(jnp.int32, shape, axis)


def dot_t(a, b):
    return lax.dot_general(a, b, (((1,), (1,)), ((), ())), preferred_element_type=F32)


def dot(a, b):
    return jnp.dot(a, b, preferred_element_type=F32)


def kernel(
    n, reach, tok_hbm, doc_hbm, pick_hbm, wq_hbm, wk_hbm, wv_hbm, wo_hbm, inner_hbm, outer_hbm, out,
    tok, doc, pick, wq, wkv, wo, inner, outer, names, names_in, kv_own, pack, hot_in, ids, ids_in,
    q_all, acc, top, att, att_in, partial, load_sem, name_s, name_r, hot_s, hot_r, ids_s, ids_r, att_s, att_r,
):
    kv = lax.axis_index("kv")
    tp = lax.axis_index("tp")
    rows = tok.shape[0]
    blocks = rows // BLOCK
    heads = wq.shape[1] // HEAD_DIM
    wide = names.shape[1]
    mine = wo.shape[1]

    barrier = pltpu.get_barrier_semaphore()

    before = jnp.minimum(kv, reach)
    after = jnp.minimum(n - 1 - kv, reach)

    def greet(d, _):
        @pl.when(d != kv)
        def _():
            pl.semaphore_signal(barrier, inc=1, device_id={"kv": d}, device_id_type=MESH)
        return 0

    lax.fori_loop(kv - before, kv + after + 1, greet, 0)
    pl.semaphore_signal(barrier, inc=1, device_id={"tp": 1 - tp}, device_id_type=MESH)

    pairs = [
        (pick_hbm, pick), (doc_hbm, doc), (tok_hbm.at[0], tok), (wk_hbm, wkv.at[:, 0:LANES]), (wv_hbm, wkv.at[:, LANES:]),
        (inner_hbm, inner), (outer_hbm.at[kv], outer), (wq_hbm, wq),
        (wo_hbm.at[pl.ds(tp * mine, mine)], wo.at[0]), (wo_hbm.at[pl.ds((1 - tp) * mine, mine)], wo.at[1]),
    ]
    loads = [pltpu.make_async_copy(a, b, load_sem.at[i]) for i, (a, b) in enumerate(pairs)]
    for load in loads:
        load.start()
    l_pick, l_doc, l_tok, l_wk, l_wv, l_in, l_out, l_wq, l_wo0, l_wo1 = loads

    l_pick.wait()
    slots = jnp.concatenate([pick[b] for b in range(blocks)], axis=0)
    block_ids = iota((blocks, wide), 1)
    hit = slots[:, 0:1] == block_ids
    for s in range(1, slots.shape[1]):
        hit = hit | (slots[:, s:s + 1] == block_ids)
    named_any = jnp.max(jnp.where(hit, 1.0, 0.0), axis=0, keepdims=True)
    names[...] = jnp.broadcast_to(named_any, names.shape)

    pl.semaphore_wait(barrier, before + after + 1)

    def name_copy(i):
        return pltpu.make_async_remote_copy(
            src_ref=names, dst_ref=names_in.at[i], send_sem=name_s.at[i], recv_sem=name_r.at[i],
            device_id={"kv": kv - 1 - i}, device_id_type=MESH)

    def name_send(i, _):
        name_copy(i).start()
        return 0

    lax.fori_loop(0, before, name_send, 0)

    def clear(i, _):
        hot_in[i] = jnp.zeros(hot_in.shape[1:], BF16)
        ids_in[i] = jnp.zeros(ids_in.shape[1:], F32)
        return 0

    lax.fori_loop(before, reach, clear, 0)

    l_in.wait()
    l_out.wait()
    cos_o, sin_o = outer[0:1, :], outer[1:2, :]
    cos_i, sin_i = inner[0], inner[1]
    cosine = cos_o * cos_i - sin_o * sin_i
    sine = sin_o * cos_i + cos_o * sin_i
    lane = iota((rows, LANES), 1)
    low = lane < HEAD_DIM
    first = lane % HEAD_DIM < HEAD_DIM // 2
    quarter = HEAD_DIM // 2

    def rotate(x):
        other = jnp.where(first, pltpu.roll(x, LANES - quarter, 1), pltpu.roll(x, quarter, 1))
        return x * cosine + other * sine

    def swap(x):
        return pltpu.roll(x, HEAD_DIM, 1)

    l_tok.wait()
    l_wk.wait()
    l_wv.wait()
    both = dot(tok[...], wkv[...])
    keys = rotate(both[:, 0:LANES])
    values = both[:, LANES:]
    is_first = tp == 0
    keys = jnp.where(is_first, keys, swap(keys))
    values = jnp.where(is_first, swap(values), values)
    packed = jnp.where(low, keys, values).astype(BF16)
    kv_own[...] = packed

    l_wq.wait()
    queries = dot(tok[...], wq[...])
    for p in range(heads // 2):
        turned = rotate(queries[:, p * LANES:(p + 1) * LANES])
        q_all[2 * p * rows:(2 * p + 1) * rows, :] = jnp.where(low, turned, 0.0).astype(BF16)
        q_all[(2 * p + 1) * rows:(2 * p + 2) * rows, :] = jnp.where(low, swap(turned), 0.0).astype(BF16)

    def name_take(i, total):
        name_copy(i).wait_recv()
        return total + names_in[i]

    total = lax.fori_loop(0, after, name_take, jnp.zeros(names.shape, F32))
    flags = jnp.broadcast_to(jnp.where(total > 0.0, 1.0, 0.0), (8, wide)).astype(BF16)
    j = iota((wide, rows), 0) - kv * blocks
    col = iota((wide, rows), 1) // BLOCK
    here = dot(flags, jnp.where(j == col, 1.0, 0.0).astype(BF16))[0:1, :]
    rank = dot(flags, jnp.where((j >= 0) & (j < col), 1.0, 0.0).astype(BF16))[0:1, :]
    kept = HOT * BLOCK
    slot = iota((2 * kept, rows), 0) % kept
    own = iota((2 * kept, rows), 1)
    choose = (here > 0.5) & (rank == (slot // BLOCK).astype(F32)) & (own % BLOCK == slot % BLOCK)
    choose = jnp.where(choose, 1.0, 0.0).astype(BF16)
    label = (iota((16, rows), 1) // BLOCK + 1).astype(F32).astype(BF16)
    pack[...] = dot(choose[0:kept], packed).astype(BF16)
    ids[...] = dot_t(label, choose)[0:1, :]

    def hot_copy(i):
        return pltpu.make_async_remote_copy(
            src_ref=pack, dst_ref=hot_in.at[i], send_sem=hot_s.at[i], recv_sem=hot_r.at[i],
            device_id={"kv": kv + 1 + i}, device_id_type=MESH)

    def ids_copy(i):
        return pltpu.make_async_remote_copy(
            src_ref=ids, dst_ref=ids_in.at[i], send_sem=ids_s.at[i], recv_sem=ids_r.at[i],
            device_id={"kv": kv + 1 + i}, device_id_type=MESH)

    def hot_send(i, _):
        ids_copy(i).start()
        hot_copy(i).start()
        return 0

    lax.fori_loop(0, after, hot_send, 0)

    l_doc.wait()
    q_pos = kv * rows + iota((rows, 1), 0)
    q_start = jnp.zeros((rows, 1), jnp.int32)
    end = jnp.int32(0)
    for i in range(doc.shape[1]):
        end = end + doc[0, i]
        q_start = jnp.where(q_pos >= end, end, q_start)

    def bias_of(key_block, key_pos):
        hits = slots[:, 0:1] == key_block
        for s in range(1, slots.shape[1]):
            hits = hits | (slots[:, s:s + 1] == key_block)
        allowed = jnp.where(hits, 0.0, -jnp.inf)
        parts = []
        for b in range(blocks):
            span = slice(b * BLOCK, (b + 1) * BLOCK)
            seen = (key_pos <= q_pos[span]) & (key_pos >= q_start[span])
            parts.append(jnp.where(seen, allowed[b:b + 1, :], -jnp.inf))
        return jnp.concatenate(parts, axis=0)

    def with_ones(block):
        return jnp.where(iota(block.shape, 1) < HEAD_DIM, jnp.ones((), BF16), block)

    local_col = iota((1, rows), 1)
    bias = bias_of(kv * blocks + local_col // BLOCK, kv * rows + local_col)
    both = jnp.concatenate([bias, bias], axis=0)
    ones_values = with_ones(packed)
    for p in range(heads // 2):
        span = slice(2 * p * rows, (2 * p + 2) * rows)
        scores = dot_t(q_all[span, :], packed) * SCALE + both
        highest = jnp.max(scores, axis=-1, keepdims=True)
        weights = jnp.exp2(scores - highest).astype(BF16)
        acc[span, :] = dot(weights, ones_values)
        top[span, :] = jnp.broadcast_to(highest, (2 * rows, LANES))

    def att_copy(h):
        return pltpu.make_async_remote_copy(
            src_ref=att.at[h], dst_ref=att_in.at[h], send_sem=att_s.at[h], recv_sem=att_r.at[h],
            device_id={"tp": 1 - tp}, device_id_type=MESH)

    def ids_wait(i, _):
        ids_copy(i).wait_recv()
        return 0

    def hot_wait(i, _):
        hot_copy(i).wait_recv()
        return 0

    senders = before
    lax.fori_loop(0, senders, ids_wait, 0)
    near = math.gcd(reach, 8)
    width = att.shape[2]

    def group(g, last):
        start = g * near
        upper = iota((1, LANES), 1) < kept
        found = []
        for i in range(0, near, 2):
            base = (kv - 1 - start - i) * blocks - 1
            even = ids_in[start + i].astype(jnp.int32)
            odd = ids_in[start + i + 1].astype(jnp.int32)
            even = jnp.where(even > 0, base + even, -2)
            odd = jnp.where(odd > 0, base - blocks + odd, -2)
            found.append(jnp.where(upper, even, odd))
        key_block = jnp.concatenate(found, axis=1)
        key_pos = key_block * BLOCK + iota((1, near * kept), 1) % BLOCK
        bias = bias_of(key_block, key_pos)
        both = jnp.concatenate([bias, bias], axis=0)
        lax.fori_loop(start, jnp.clip(senders, start, start + near), hot_wait, 0)
        block = hot_in[pl.ds(start, near)].reshape(near * kept, LANES)
        ones_values = with_ones(block)
        for p in range(heads // 2):
            span = slice(2 * p * rows, (2 * p + 2) * rows)
            scores = dot_t(q_all[span, :], block) * SCALE + both
            before = top[span, :]
            highest = jnp.maximum(before, jnp.max(scores, axis=-1, keepdims=True))
            weights = jnp.exp2(scores - highest[:, 0:1]).astype(BF16)
            summed = acc[span, :] * jnp.exp2(before - highest) + dot(weights, ones_values)
            if not last:
                acc[span, :] = summed
                top[span, :] = highest
                continue
            even, odd = summed[0:rows], summed[rows:]
            above = jnp.where(low, swap(even), odd)
            below = jnp.where(low, even, swap(odd))
            half, place = divmod(p * LANES, width)
            att[half, :, place:place + LANES] = (above / below).astype(BF16)
            if place + LANES == width:
                att_copy(half).start()

    if reach > near:
        def step(g, _):
            group(g, False)
            return 0

        lax.fori_loop(0, reach // near - 1, step, 0)
    group(reach // near - 1, True)

    l_wo0.wait()
    halves = att.shape[0]
    columns = wo.shape[2]
    piece = columns // 4
    for c in range(4):
        cut = slice(c * piece, (c + 1) * piece)
        value = dot(att[0], wo[0, 0:width, cut])
        for h in range(1, halves):
            value += dot(att[h], wo[0, h * width:(h + 1) * width, cut])
        partial[:, cut] = value
    l_wo1.wait()
    for h in range(halves):
        att_copy(h).wait_recv()
    for c in range(4):
        cut = slice(c * piece, (c + 1) * piece)
        value = partial[:, cut]
        for h in range(halves):
            value += dot(att_in[h], wo[1, h * width:(h + 1) * width, cut])
        out[0, :, cut] = value.astype(BF16)

    def name_done(i, _):
        name_copy(i).wait_send()
        return 0

    def hot_done(i, _):
        ids_copy(i).wait_send()
        hot_copy(i).wait_send()
        return 0

    lax.fori_loop(0, before, name_done, 0)
    lax.fori_loop(0, after, hot_done, 0)
    for h in range(halves):
        att_copy(h).wait_send()


def solution(mesh):
    n = mesh.shape["kv"]

    def shards(tokens, doc_lengths, picked, w_query, w_key, w_value, w_out):
        _, rows, d = tokens.shape
        blocks = rows // BLOCK
        wide = -(-n * blocks // LANES) * LANES
        q_cols = w_query.shape[1]
        heads = q_cols // HEAD_DIM
        columns = w_out.shape[1]
        inner, outer = tables(rows, n)
        width = q_cols // 2
        dma = pltpu.SemaphoreType.DMA
        payload = HOT * BLOCK
        reach = min(n, (n * rows // 2 + rows - 2) // rows)
        reach += reach % 2
        operands = (tokens, doc_lengths, jnp.transpose(picked, (1, 0, 2)), w_query, w_key, w_value, w_out, inner, outer)
        operands = [pltpu.with_memory_space_constraint(jnp.asarray(x), pltpu.HBM) for x in operands]
        return pl.pallas_call(
            functools.partial(kernel, n, reach),
            out_shape=jax.ShapeDtypeStruct((1, rows, columns), BF16),
            in_specs=[pl.BlockSpec(memory_space=pltpu.HBM)] * 9,
            out_specs=pl.BlockSpec(memory_space=pltpu.VMEM),
            scratch_shapes=[
                pltpu.VMEM((rows, d), BF16),
                pltpu.SMEM(doc_lengths.shape, jnp.int32),
                pltpu.VMEM((blocks, 1, picked.shape[2]), jnp.int32),
                pltpu.VMEM(w_query.shape, BF16),
                pltpu.VMEM((d, 2 * LANES), BF16),
                pltpu.VMEM((2, w_out.shape[0] // 2, columns), BF16),
                pltpu.VMEM(inner.shape, F32),
                pltpu.VMEM(outer.shape[1:], F32),
                pltpu.VMEM((1, wide), F32),
                pltpu.VMEM((reach, 1, wide), F32),
                pltpu.VMEM((rows, LANES), BF16),
                pltpu.VMEM((payload, LANES), BF16),
                pltpu.VMEM((reach, payload, LANES), BF16),
                pltpu.VMEM((1, LANES), F32),
                pltpu.VMEM((reach, 1, LANES), F32),
                pltpu.VMEM((heads * rows, LANES), BF16),
                pltpu.VMEM((heads * rows, LANES), F32),
                pltpu.VMEM((heads * rows, LANES), F32),
                pltpu.VMEM((2, rows, width), BF16),
                pltpu.VMEM((2, rows, width), BF16),
                pltpu.VMEM((rows, columns), F32),
                dma((10,)), *[dma((reach,))] * 6, dma((2,)), dma((2,)),
            ],
            compiler_params=pltpu.CompilerParams(
                collective_id=0, has_side_effects=True, vmem_limit_bytes=24 * 1024 * 1024
            ),
        )(*operands)

    placed = (P("dp", "kv", None), P("dp", None), P("dp", "kv", None), P(None, "tp"), P(), P(), P())
    return jax.shard_map(
        shards, mesh=mesh, in_specs=placed, out_specs=P("dp", "kv", None), check_vma=False
    )
```
